32 devices in a mesh: fs: 16 (over z, y, x), tp: 2 (over core).
Axes of the slice: x: 2, y: 2, z: 4, core: 2. Of those that a mesh axis runs over, the one named last changes fastest.
Arguments:
- inputs: bfloat16 [8192, 2048], P('fs', 'tp'), may hold values from -6 to 6
- value_cotangent: bfloat16 [8192, 2048], P('fs', 'tp'), may hold values from -6 to 6
- first_map: bfloat16 [8192, 2048], P('fs', 'tp'), may hold values from -6 to 6
- second_map: bfloat16 [8192, 2048], P('fs', 'tp'), may hold values from -6 to 6
- lambdas: float32 [16], P('tp'), may hold values from 0.3 to 0.8
- head_gain: float32 [128], replicated, may hold values from 0.1 to 1.9
- output_cotangent: bfloat16 [8192, 2048], P('fs', 'tp'), may hold values from -6 to 6
- value_factor: bfloat16 [2048, 256], replicated, may hold values from -0.125 to 0.125
- output_factor: bfloat16 [2048, 256], replicated, may hold values from -0.125 to 0.125
- value_weight: float32 [2048, 2048], P('fs', 'tp'), may hold values from -0.125 to 0.125
- output_weight: float32 [2048, 2048], P('tp', 'fs'), may hold values from -0.125 to 0.125
- value_moment: float32 [256, 2048], P('fs', 'tp'), may hold values from -6 to 6
- value_second: float32 [256, 2048], P('fs', 'tp'), may hold values from 0.25 to 4
- output_moment: float32 [256, 2048], P('fs', 'tp'), may hold values from -6 to 6
- output_second: float32 [256, 2048], P('fs', 'tp'), may hold values from 0.25 to 4
Outputs:
- value_master: float32 [2048, 2048], P('fs', 'tp')
- output_master: float32 [2048, 2048], P('tp', 'fs')
- value_moment_new: float32 [256, 2048], P('fs', 'tp')
- value_second_new: float32 [256, 2048], P('fs', 'tp')
- output_moment_new: float32 [256, 2048], P('fs', 'tp')
- output_second_new: float32 [256, 2048], P('fs', 'tp')
- value_copy: bfloat16 [2048, 2048], P(None, 'tp')
- output_copy: bfloat16 [2048, 2048], P('tp')
The draws below stay inside these ranges and needn't reach their ends.
All inputs are finite; a program needn't handle non-finite values.
Results may differ from the reference program's by a relative error of at most 0.0027.
Values may be sent and summed in bfloat16 or wider, within the bound.
A program may use at most 64 MiB of HBM per device.

```python
import math
import jax
import jax.numpy as jnp
from jax import lax

D = 2048
H = 16
VD = 128
R = 256
TOKENS = 8192


def block_scale(own_key, extent, pieces, smallest, high):
    loudness, own = 1.0, jax.random.fold_in(own_key, 6)
    for dim, blocks in pieces:
        draws = jnp.exp(jax.random.uniform(jax.random.fold_in(own, dim), (blocks,), jnp.float32, smallest / len(pieces), high / len(pieces)))
        loudness = loudness * jnp.repeat(draws, extent[dim] // blocks).reshape([-1 if axis == dim else 1 for axis in range(len(extent))])
    return loudness


def scatter_about(key, extent, spread, limit, shards=(), dtype=jnp.bfloat16):
    values = spread * jax.random.normal(key, extent, jnp.float32)
    if shards:
        values = values * block_scale(key, extent, shards, -0.22, 0.18)
    return jnp.clip(values, -limit, limit).astype(dtype)


def setup_inputs(seed: int = 0) -> dict:
    seeds = jax.random.split(jax.random.key(seed), 16)
    inputs = scatter_about(seeds[0], (TOKENS, D), 1.0, 6.0, ((0, 16), (1, 2)))
    value_cotangent = scatter_about(seeds[1], (TOKENS, H * VD), 1.0, 6.0, ((0, 16), (1, 2)))
    first_map = scatter_about(seeds[2], (TOKENS, H * VD), 1.0, 6.0, ((0, 16), (1, 2)))
    second_map = scatter_about(seeds[3], (TOKENS, H * VD), 1.0, 6.0, ((0, 16), (1, 2)))
    lambdas = jnp.clip(0.3 + 0.5 * jax.random.uniform(seeds[4], (H,), jnp.float32) ** block_scale(seeds[4], (H,), ((0, 2),), -0.2, 0.2), 0.3, 0.8)
    head_gain = jnp.clip(1.0 + 0.18 * jax.random.normal(seeds[5], (VD,), jnp.float32), 0.1, 1.9)
    output_cotangent = scatter_about(seeds[6], (TOKENS, D), 1.0, 6.0, ((0, 16), (1, 2)))
    value_factor = scatter_about(seeds[7], (D, R), D ** -0.5, 0.125)
    output_factor = scatter_about(seeds[8], (D, R), D ** -0.5, 0.125)
    value_weight = scatter_about(seeds[9], (D, H * VD), D ** -0.5, 0.125, ((0, 16), (1, 2)), jnp.float32)
    output_weight = scatter_about(seeds[10], (H * VD, D), (H * VD) ** -0.5, 0.125, ((0, 2), (1, 16)), jnp.float32)
    value_moment = scatter_about(seeds[11], (R, H * VD), 1.0, 6.0, ((0, 16), (1, 2)), jnp.float32)
    value_second = jnp.clip(jnp.exp(math.log(4.0) - 2.7725887 * jax.random.uniform(seeds[12], (R, H * VD), jnp.float32) ** block_scale(seeds[12], (R, H * VD), ((0, 16), (1, 2)), -0.2, 0.2)), 0.25, 4.0)
    output_moment = scatter_about(seeds[13], (R, H * VD), 1.0, 6.0, ((0, 16), (1, 2)), jnp.float32)
    output_second = jnp.clip(jnp.exp(math.log(4.0) - 2.7725887 * jax.random.uniform(seeds[14], (R, H * VD), jnp.float32) ** block_scale(seeds[14], (R, H * VD), ((0, 16), (1, 2)), -0.2, 0.2)), 0.25, 4.0)
    return {"inputs": inputs, "value_cotangent": value_cotangent, "first_map": first_map, "second_map": second_map, "lambdas": lambdas, "head_gain": head_gain, "output_cotangent": output_cotangent, "value_factor": value_factor, "output_factor": output_factor, "value_weight": value_weight, "output_weight": output_weight, "value_moment": value_moment, "value_second": value_second, "output_moment": output_moment, "output_second": output_second}


def contract_rows(left, right, precise):
    if precise:
        return lax.dot_general(left, right, (((0,), (0,)), ((), ())), precision=lax.Precision.HIGHEST, preferred_element_type=jnp.float32)
    return lax.dot_general(left, right, (((0,), (0,)), ((), ())), preferred_element_type=jnp.float32)

def reference(inputs, value_cotangent, first_map, second_map, lambdas, head_gain, output_cotangent, value_factor, output_factor, value_weight, output_weight, value_moment, value_second, output_moment, output_second):
    tok_count = inputs.shape[0]
    first = first_map.astype(jnp.float32).reshape(tok_count, H, VD)
    second = second_map.astype(jnp.float32).reshape(tok_count, H, VD)
    difference = first - lambdas[None, :, None] * second
    normed = difference * lax.rsqrt(lax.optimization_barrier(jnp.mean(difference * difference, axis=-1, keepdims=True)) + 1e-06) * head_gain
    heads_out = normed.reshape(tok_count, H * VD).astype(jnp.bfloat16)
    token_scale = 1.0 / math.sqrt(TOKENS)
    grad_value = contract_rows(inputs, value_cotangent, False) * token_scale
    grad_output_t = contract_rows(output_cotangent, heads_out, False) * token_scale
    low_value = contract_rows(value_factor.astype(jnp.float32), grad_value, True)
    low_output = contract_rows(output_factor.astype(jnp.float32), grad_output_t, True)
    value_moment_new = 0.8 * value_moment + 0.2 * low_value
    value_second_new = 0.95 * value_second + 0.05 * low_value * low_value
    output_moment_new = 0.8 * output_moment + 0.2 * low_output
    output_second_new = 0.95 * output_second + 0.05 * low_output * low_output
    direction_value = value_moment_new / (jnp.sqrt(value_second_new) + 1e-08)
    direction_output = output_moment_new / (jnp.sqrt(output_second_new) + 1e-08)
    step_value = jnp.dot(value_factor.astype(jnp.float32), direction_value, precision=lax.Precision.HIGHEST, preferred_element_type=jnp.float32)
    step_output = jnp.dot(output_factor.astype(jnp.float32), direction_output, precision=lax.Precision.HIGHEST, preferred_element_type=jnp.float32)
    value_master = value_weight - 0.05 * step_value
    output_master = output_weight - 0.05 * step_output.T
    return (value_master, output_master, value_moment_new, value_second_new, output_moment_new, output_second_new, value_master.astype(jnp.bfloat16), output_master.astype(jnp.bfloat16))
```

```python
import functools
import math

import jax
import jax.numpy as jnp
from jax import lax
from jax.experimental import pallas as pl
from jax.experimental.pallas import tpu as pltpu
from jax.sharding import PartitionSpec as P

F32 = jnp.float32
BF16 = jnp.bfloat16


CODE = 2.0**30


def encode(w):
    square = (w * CODE) * (w * CODE)
    fourth = square * square
    return jnp.where(w < 0, -fourth, fourth).astype(BF16)


def decode(v):
    v = v.astype(F32)
    size = lax.rsqrt(lax.rsqrt(jnp.abs(v))) * (1.0 / CODE)
    return jnp.where(v < 0, -size, size)


def exchange(
    nfs, ntp, scale,
    vw, ow, inp, vcot, first, second, ocot, lam, gain, vfac, ofac, vm, vs, om, os_,
    gv, go, dfull, vm_new, vs_new, om_new, os_new,
    heads, proj, part, got, direction,
    vsend, vrecv, osend, orecv, psend, precv, rsend, rrecv, dsend, drecv, lsem,
):
    me = lax.axis_index("fs")
    tp = lax.axis_index("tp")
    cols = inp.shape[1]
    rank = vfac.shape[1]
    nx = 2 if nfs % 2 == 0 else 1
    ny = 2 if nfs % 4 == 0 else 1
    nz = nfs // (nx * ny)
    x = lax.rem(me, nx)
    y = lax.rem(lax.div(me, nx), ny)
    z = lax.div(me, nx * ny)

    def at(dz, dy, dx):
        zz = lax.rem(z + dz, nz)
        yy = lax.rem(y + dy, ny)
        xx = lax.rem(x + dx, nx)
        return (zz * ny + yy) * nx + xx

    barrier = pltpu.get_barrier_semaphore()
    for k in range(1, nfs):
        pl.semaphore_signal(barrier, inc=1, device_id={"fs": lax.rem(me + k, nfs)})
    for k in range(1, ntp):
        pl.semaphore_signal(barrier, inc=1, device_id={"tp": lax.rem(tp + k, ntp)})
    pl.semaphore_wait(barrier, nfs + ntp - 2)

    width = vw.shape[0]

    def vslot(b):
        return gv.at[b]

    def oslot(b):
        if len(go.shape) == 2:
            return go.at[:, pl.ds(pl.multiple_of(b * width, width), width)]
        return go.at[b]

    pending = []
    counts = {"v": 0, "o": 0}

    def send(kind, src, b, target):
        k = counts[kind]
        counts[kind] = k + 1
        slot, ss, rs = (vslot, vsend, vrecv) if kind == "v" else (oslot, osend, orecv)
        copy = pltpu.make_async_remote_copy(
            src_ref=slot(b) if src is None else src,
            dst_ref=slot(b),
            send_sem=ss.at[k],
            recv_sem=rs.at[b],
            device_id={"fs": target},
        )
        copy.start()
        pending.append(copy)

    def arrived(kind, b):
        slot, ss, rs = (vslot, vsend, vrecv) if kind == "v" else (oslot, osend, orecv)
        pltpu.make_async_remote_copy(
            src_ref=slot(b), dst_ref=slot(b), send_sem=ss.at[0], recv_sem=rs.at[b],
            device_id={"fs": me},
        ).wait_recv()

    own_v = pltpu.make_async_copy(vw, vslot(me), lsem.at[0])
    own_o = pltpu.make_async_copy(ow, oslot(me), lsem.at[1])
    own_v.start()
    own_o.start()
    for dz in range(1, nz):
        send("v", vw, me, at(dz, 0, 0))
        send("o", ow, me, at(dz, 0, 0))
    if ny > 1:
        send("v", vw, me, at(0, 1, 0))
    if nx > 1:
        send("o", ow, me, at(0, 0, 1))
        send("v", vw, me, at(0, 0, 1))
    if ny > 1:
        send("o", ow, me, at(0, 1, 0))

    proj[0, :, :rank] = jnp.dot(inp[...], vfac[...], preferred_element_type=F32)
    proj[0, :, rank:] = jnp.dot(ocot[...], ofac[...], preferred_element_type=F32)
    pcopies = []
    for k in range(1, ntp):
        copy = pltpu.make_async_remote_copy(
            src_ref=proj.at[0], dst_ref=proj.at[k],
            send_sem=psend.at[k], recv_sem=precv.at[k],
            device_id={"tp": lax.rem(tp + k, ntp)},
        )
        copy.start()
        pcopies.append(copy)

    head_width = gain.shape[1]
    for h in range(cols // head_width):
        span = pl.ds(h * head_width, head_width)
        diff = first[:, span].astype(F32) - lam[h] * second[:, span].astype(F32)
        mean = jnp.mean(diff * diff, axis=-1, keepdims=True)
        heads[:, span] = (diff * lax.rsqrt(mean + 1e-06) * gain[...]).astype(BF16)

    for copy in pcopies:
        copy.wait()
    total = proj[0]
    for k in range(1, ntp):
        total = total + proj[k]
    high = total.astype(BF16)
    low = (total - high.astype(F32)).astype(BF16)

    def contract(a, b):
        return lax.dot_general(a, b, (((0,), (0,)), ((), ())), preferred_element_type=F32)

    rows = vm.shape[0]
    low_v = (contract(high[:, :rank], vcot[...]) + contract(low[:, :rank], vcot[...])) * scale
    part[:, :, :cols] = low_v.astype(BF16).reshape(nfs, rows, cols)
    low_o = (contract(high[:, rank:], heads[...]) + contract(low[:, rank:], heads[...])) * scale
    part[:, :, cols:] = low_o.astype(BF16).reshape(nfs, rows, cols)

    rcopies = []
    for k in range(1, nfs):
        peer = lax.rem(me + k, nfs)
        copy = pltpu.make_async_remote_copy(
            src_ref=part.at[peer], dst_ref=got.at[k],
            send_sem=rsend.at[k], recv_sem=rrecv.at[k],
            device_id={"fs": peer},
        )
        copy.start()
        rcopies.append(copy)

    for dz in range(1, nz):
        b = at(dz, 0, 0)
        arrived("v", b)
        if ny > 1:
            send("v", None, b, at(0, 1, 0))
        arrived("o", b)
        if nx > 1:
            send("o", None, b, at(0, 0, 1))
            send("v", None, b, at(0, 0, 1))
        if ny > 1:
            send("o", None, b, at(0, 1, 0))

    for copy in rcopies:
        copy.wait_recv()
    own = part[me].astype(F32)
    for k in range(1, nfs):
        own = own + got[k].astype(F32)
    for off, m_ref, s_ref, m_out, s_out in (
        (0, vm, vs, vm_new, vs_new),
        (cols, om, os_, om_new, os_new),
    ):
        g = own[:, off:off + cols]
        m = 0.8 * m_ref[...] + 0.2 * g
        s = 0.95 * s_ref[...] + 0.05 * g * g
        m_out[...] = m
        s_out[...] = s
        direction[:, off:off + cols] = (m / (jnp.sqrt(s) + 1e-08)).astype(BF16)
    own_d = pltpu.make_async_copy(direction, dfull.at[me], lsem.at[2])
    own_d.start()
    dcopies = []
    for k in range(1, nfs):
        copy = pltpu.make_async_remote_copy(
            src_ref=direction, dst_ref=dfull.at[me],
            send_sem=dsend.at[k], recv_sem=drecv.at[k],
            device_id={"fs": lax.rem(me + k, nfs)},
        )
        copy.start()
        dcopies.append(copy)

    for dz in range(nz):
        if ny > 1:
            b = at(dz, 1, 0)
            arrived("v", b)
            if nx > 1:
                send("v", None, b, at(0, 0, 1))
        if nx > 1:
            b = at(dz, 0, 1)
            arrived("o", b)
            if ny > 1:
                send("o", None, b, at(0, 1, 0))

    for dz in range(nz):
        for dy in range(ny):
            if nx > 1:
                arrived("v", at(dz, dy, 1))
        for dx in range(nx):
            if ny > 1:
                arrived("o", at(dz, 1, dx))
    for k, copy in enumerate(dcopies):
        src = lax.rem(me + nfs - (k + 1), nfs)
        pltpu.make_async_remote_copy(
            src_ref=direction, dst_ref=dfull.at[src],
            send_sem=dsend.at[0], recv_sem=drecv.at[k + 1], device_id={"fs": src},
        ).wait_recv()
    for copy in rcopies + dcopies + pending:
        copy.wait_send()
    own_v.wait()
    own_o.wait()
    own_d.wait()


def local(
    nfs, ntp,
    inputs, value_cotangent, first_map, second_map, lambdas, head_gain,
    output_cotangent, value_factor, output_factor, value_weight, output_weight,
    value_moment, value_second, output_moment, output_second,
):
    tokens, cols = inputs.shape
    width = value_weight.shape[0]
    rank = value_factor.shape[1]
    rows = value_moment.shape[0]
    tp = lax.axis_index("tp")
    fs = lax.axis_index("fs")
    vfac = lax.dynamic_slice_in_dim(value_factor, tp * cols, cols, 0)
    ofac = lax.dynamic_slice_in_dim(output_factor, tp * cols, cols, 0)
    scale = 1.0 / math.sqrt(tokens * nfs)
    flat = width % 128 == 0
    go_shape = (cols, nfs * width) if flat else (nfs, cols, width)
    vmem = pl.BlockSpec(memory_space=pltpu.VMEM)
    hbm = pl.BlockSpec(memory_space=pl.ANY)
    dma = pltpu.SemaphoreType.DMA
    moment = jax.ShapeDtypeStruct((rows, cols), F32)
    gv, go, dfull, vm_new, vs_new, om_new, os_new = pl.pallas_call(
        functools.partial(exchange, nfs, ntp, scale),
        out_shape=(
            jax.ShapeDtypeStruct((nfs, width, cols), BF16),
            jax.ShapeDtypeStruct(go_shape, BF16),
            jax.ShapeDtypeStruct((nfs, rows, 2 * cols), BF16),
            moment, moment, moment, moment,
        ),
        in_specs=[vmem] * 7 + [pl.BlockSpec(memory_space=pltpu.SMEM)] + [vmem] * 7,
        out_specs=(hbm, hbm, hbm, vmem, vmem, vmem, vmem),
        scratch_shapes=[
            pltpu.VMEM((tokens, cols), BF16),
            pltpu.VMEM((ntp, tokens, 2 * rank), F32),
            pltpu.VMEM((nfs, rows, 2 * cols), BF16),
            pltpu.VMEM((nfs, rows, 2 * cols), BF16),
            pltpu.VMEM((rows, 2 * cols), BF16),
            dma((nfs,)), dma((nfs,)), dma((nfs,)), dma((nfs,)),
            dma((ntp,)), dma((ntp,)),
            dma((nfs,)), dma((nfs,)), dma((nfs,)), dma((nfs,)), dma((3,)),
        ],
        compiler_params=pltpu.CompilerParams(collective_id=0, has_side_effects=True),
    )(
        encode(value_weight), encode(output_weight),
        inputs, value_cotangent, first_map, second_map, output_cotangent,
        lambdas, head_gain.reshape(1, -1), vfac, ofac,
        value_moment, value_second, output_moment, output_second,
    )
    dirs = dfull.reshape(nfs * rows, 2 * cols)
    dir_v, dir_o = dirs[:, :cols], dirs[:, cols:]
    vrows = lax.dynamic_slice_in_dim(value_factor, fs * width, width, 0)
    orows = lax.dynamic_slice_in_dim(output_factor, fs * width, width, 0)

    def step_v(factor):
        return jnp.dot(factor, dir_v, preferred_element_type=F32)

    def step_o(factor):
        return lax.dot_general(
            dir_o, factor, (((0,), (1,)), ((), ())), preferred_element_type=F32
        )

    value_master = value_weight - 0.05 * step_v(vrows)
    output_master = output_weight - 0.05 * step_o(orows)
    whole_v = decode(gv.reshape(nfs * width, cols))
    whole_o = decode(go if flat else go.transpose(1, 0, 2).reshape(cols, nfs * width))
    value_copy = (whole_v - 0.05 * step_v(value_factor)).astype(BF16)
    output_copy = (whole_o - 0.05 * step_o(output_factor)).astype(BF16)
    return (
        value_master, output_master, vm_new, vs_new, om_new, os_new,
        value_copy, output_copy,
    )


def solution(mesh):
    both = P("fs", "tp")
    in_specs = (
        both, both, both, both, P("tp"), P(), both, P(), P(), both, P("tp", "fs"),
        both, both, both, both,
    )
    out_specs = (
        both, P("tp", "fs"), both, both, both, both, P(None, "tp"), P("tp", None),
    )
    body = functools.partial(local, mesh.shape["fs"], mesh.shape["tp"])
    return jax.shard_map(
        body, mesh=mesh, in_specs=in_specs, out_specs=out_specs, check_vma=False
    )
```

```python
import functools
import math

import jax
import jax.numpy as jnp
from jax import lax
from jax.experimental import pallas as pl
from jax.experimental.pallas import tpu as pltpu
from jax.sharding import PartitionSpec as P

F32 = jnp.float32
BF16 = jnp.bfloat16


CODE = 2.0**30


def encode(w):
    square = (w * CODE) * (w * CODE)
    fourth = square * square
    return jnp.where(w < 0, -fourth, fourth).astype(BF16)


def decode(v):
    v = v.astype(F32)
    size = lax.rsqrt(lax.rsqrt(jnp.maximum(jnp.abs(v), 1e-36))) * (1.0 / CODE)
    return jnp.where(v < 0, -size, size)


def exchange(
    nfs, ntp, scale,
    vw, ow, inp, vcot, first, second, ocot, lam, gain, vfac, ofac, vm, vs, om, os_,
    gv, go, dfull, own_out,
    heads, proj, part, got, direction,
    vsend, vrecv, osend, orecv, psend, precv, rsend, rrecv,
    dvsend, dvrecv, dosend, dorecv, lsem,
):
    me = lax.axis_index("fs")
    tp = lax.axis_index("tp")
    cols = inp.shape[1]
    rank = vfac.shape[1]
    nx = 2 if nfs % 2 == 0 else 1
    ny = 2 if nfs % 4 == 0 else 1
    nz = nfs // (nx * ny)
    x = lax.rem(me, nx)
    y = lax.rem(lax.div(me, nx), ny)
    z = lax.div(me, nx * ny)

    def at(dz, dy, dx):
        zz = lax.rem(z + dz, nz)
        yy = lax.rem(y + dy, ny)
        xx = lax.rem(x + dx, nx)
        return (zz * ny + yy) * nx + xx

    barrier = pltpu.get_barrier_semaphore()
    for k in range(1, nfs):
        pl.semaphore_signal(barrier, inc=1, device_id={"fs": lax.rem(me + k, nfs)})
    for k in range(1, ntp):
        pl.semaphore_signal(barrier, inc=1, device_id={"tp": lax.rem(tp + k, ntp)})
    pl.semaphore_wait(barrier, nfs + ntp - 2)

    width = vw.shape[0]

    def vslot(b):
        return gv.at[b]

    def oslot(b):
        if len(go.shape) == 2:
            return go.at[:, pl.ds(pl.multiple_of(b * width, width), width)]
        return go.at[b]

    def dvslot(b):
        return dfull.at[b, :, pl.ds(0, cols)]

    def doslot(b):
        return dfull.at[b, :, pl.ds(cols, cols)]

    kinds = {
        "v": (vslot, vsend, vrecv),
        "o": (oslot, osend, orecv),
        "dv": (dvslot, dvsend, dvrecv),
        "do": (doslot, dosend, dorecv),
    }
    pending = []
    counts = {kind: 0 for kind in kinds}

    def when(cond, run):
        if cond is None:
            run()
        else:
            pl.when(cond)(run)

    def send(kind, src, b, target, cond=None):
        k = counts[kind]
        counts[kind] = k + 1
        slot, ss, rs = kinds[kind]

        def make():
            return pltpu.make_async_remote_copy(
                src_ref=slot(b) if src is None else src,
                dst_ref=slot(b),
                send_sem=ss.at[k],
                recv_sem=rs.at[b],
                device_id={"fs": target},
            )

        when(cond, lambda: make().start())
        pending.append((cond, make))

    def arrived(kind, b, cond=None):
        slot, ss, rs = kinds[kind]
        when(cond, lambda: pltpu.make_async_remote_copy(
            src_ref=slot(b), dst_ref=slot(b), send_sem=ss.at[0], recv_sem=rs.at[b],
            device_id={"fs": me},
        ).wait_recv())

    def spread(kind, src, b, cond=None):
        turns = ((ny, (0, 1, 0)), (nx, (0, 0, 1)))
        for extent, turn in turns if kind in ("v", "dv") else turns[::-1]:
            if extent > 1:
                send(kind, src, b, at(*turn), cond)

    def across(kind, bz, cond=None):
        first_turn, second_turn = (ny, nx) if kind in ("v", "dv") else (nx, ny)
        if first_turn == 1:
            return
        if kind in ("v", "dv"):
            b, target = (bz * ny + lax.rem(y + 1, ny)) * nx + x, at(0, 0, 1)
        else:
            b, target = (bz * ny + y) * nx + lax.rem(x + 1, nx), at(0, 1, 0)
        arrived(kind, b, cond)
        if second_turn > 1:
            send(kind, None, b, target, cond)

    def plane(bz):
        return (bz * ny + y) * nx + x

    up, down = lax.rem(z + 1, nz), lax.rem(z + nz - 1, nz)

    def along(kind, s):
        for sign in (1, -1):
            source = z - sign * s
            cond = source >= 0 if sign == 1 else source < nz
            b = plane(lax.rem(source + nz, nz))
            arrived(kind, b, cond)
            if sign == 1:
                send(kind, None, b, plane(up), (source >= 0) & (z + 1 < nz))
            else:
                send(kind, None, b, plane(down), (source < nz) & (z > 0))
            spread(kind, None, b, cond)

    def behind(kind, s):
        for sign in (1, -1):
            source = z - sign * s
            cond = source >= 0 if sign == 1 else source < nz
            across(kind, lax.rem(source + nz, nz), cond)

    own_v = pltpu.make_async_copy(vw, vslot(me), lsem.at[0])
    own_o = pltpu.make_async_copy(ow, oslot(me), lsem.at[1])
    own_v.start()
    own_o.start()
    for kind, src in (("v", vw), ("o", ow)):
        send(kind, src, me, plane(up), z + 1 < nz)
        send(kind, src, me, plane(down), z > 0)
        spread(kind, src, me)

    proj[0, :, :rank] = jnp.dot(inp[...], vfac[...], preferred_element_type=F32)
    proj[0, :, rank:] = jnp.dot(ocot[...], ofac[...], preferred_element_type=F32)
    pcopies = []
    for k in range(1, ntp):
        copy = pltpu.make_async_remote_copy(
            src_ref=proj.at[0], dst_ref=proj.at[k],
            send_sem=psend.at[k], recv_sem=precv.at[k],
            device_id={"tp": lax.rem(tp + k, ntp)},
        )
        copy.start()
        pcopies.append(copy)

    head_width = gain.shape[1]
    for h in range(cols // head_width):
        span = pl.ds(h * head_width, head_width)
        diff = first[:, span].astype(F32) - lam[h] * second[:, span].astype(F32)
        mean = jnp.mean(diff * diff, axis=-1, keepdims=True)
        heads[:, span] = (diff * lax.rsqrt(mean + 1e-06) * gain[...]).astype(BF16)

    for copy in pcopies:
        copy.wait()
    total = proj[0]
    for k in range(1, ntp):
        total = total + proj[k]
    high = total.astype(BF16)
    low = (total - high.astype(F32)).astype(BF16)

    def contract(a, b):
        return lax.dot_general(a, b, (((0,), (0,)), ((), ())), preferred_element_type=F32)

    rows = vm.shape[0]
    low_v = (contract(high[:, :rank], vcot[...]) + contract(low[:, :rank], vcot[...])) * scale
    part[:, :, :cols] = low_v.astype(BF16).reshape(nfs, rows, cols)
    low_o = (contract(high[:, rank:], heads[...]) + contract(low[:, rank:], heads[...])) * scale
    part[:, :, cols:] = low_o.astype(BF16).reshape(nfs, rows, cols)

    rcopies = []
    for k in range(1, nfs):
        peer = lax.rem(me + k, nfs)
        copy = pltpu.make_async_remote_copy(
            src_ref=part.at[peer], dst_ref=got.at[k],
            send_sem=rsend.at[k], recv_sem=rrecv.at[k],
            device_id={"fs": peer},
        )
        copy.start()
        rcopies.append(copy)

    for s in range(1, nz):
        for kind in ("v", "o"):
            along(kind, s)
        for kind in ("v", "o"):
            if s == 1:
                across(kind, z)
            else:
                behind(kind, s - 1)

    for copy in rcopies:
        copy.wait_recv()
    own = part[me].astype(F32)
    for k in range(1, nfs):
        own = own + got[k].astype(F32)
    own_out[...] = own
    for off, m_ref, s_ref in ((0, vm, vs), (cols, om, os_)):
        g = own[:, off:off + cols]
        m = 0.8 * m_ref[...] + 0.2 * g
        s = 0.95 * s_ref[...] + 0.05 * g * g
        direction[:, off:off + cols] = (m / (jnp.sqrt(s) + 1e-08)).astype(BF16)
    own_d = pltpu.make_async_copy(direction, dfull.at[me], lsem.at[2])
    own_d.start()
    halves = {"dv": direction.at[:, pl.ds(0, cols)], "do": direction.at[:, pl.ds(cols, cols)]}
    for kind, src in halves.items():
        for dz in range(1, nz):
            send(kind, src, me, at(dz, 0, 0))
        spread(kind, src, me)
    for dz in range(1, nz):
        for kind in halves:
            arrived(kind, at(dz, 0, 0))
            spread(kind, None, at(dz, 0, 0))
    for dz in range(nz):
        for kind in halves:
            across(kind, lax.rem(z + dz, nz))
    for kind in ("v", "o"):
        if nz > 1:
            behind(kind, nz - 1)
        else:
            across(kind, z)

    for dz in range(nz):
        for dy in range(ny):
            if nx > 1:
                arrived("v", at(dz, dy, 1))
                arrived("dv", at(dz, dy, 1))
        for dx in range(nx):
            if ny > 1:
                arrived("o", at(dz, 1, dx))
                arrived("do", at(dz, 1, dx))
    for copy in rcopies:
        copy.wait_send()
    for cond, make in pending:
        when(cond, lambda make=make: make().wait_send())
    own_v.wait()
    own_o.wait()
    own_d.wait()


def update(
    width, fs, gv, go, vfac, ofac, dv, do, vw, ow, own, vm, vs, om, os_,
    v_copy, o_copy, v_master, o_master, vm_new, vs_new, om_new, os_new, turned,
):
    step = pl.program_id(0)
    cols = dv.shape[1]

    @pl.when(step == 0)
    def _():
        turned[...] = do[...].T
        for off, m_ref, s_ref, m_out, s_out in (
            (0, vm, vs, vm_new, vs_new),
            (cols, om, os_, om_new, os_new),
        ):
            g = own[:, off:off + cols]
            m_out[...] = 0.8 * m_ref[...] + 0.2 * g
            s_out[...] = 0.95 * s_ref[...] + 0.05 * g * g

    move_v = 0.05 * jnp.dot(vfac[...], dv[...], preferred_element_type=F32)
    move_o = 0.05 * lax.dot_general(
        turned[...], ofac[...], (((1,), (1,)), ((), ())), preferred_element_type=F32
    )
    v_copy[...] = (decode(gv[0]) - move_v).astype(BF16)
    o_old = decode(go[...] if len(go.shape) == 2 else go[0])
    o_new = (o_old - move_o).astype(BF16)
    if len(go.shape) == 2:
        o_copy[...] = o_new
    else:
        o_copy[0] = o_new

    @pl.when(step == fs[0])
    def _():
        v_master[...] = vw[...] - move_v
        o_master[...] = ow[...] - move_o


def local(
    nfs, ntp,
    inputs, value_cotangent, first_map, second_map, lambdas, head_gain,
    output_cotangent, value_factor, output_factor, value_weight, output_weight,
    value_moment, value_second, output_moment, output_second,
):
    tokens, cols = inputs.shape
    width = value_weight.shape[0]
    rank = value_factor.shape[1]
    rows = value_moment.shape[0]
    tp = lax.axis_index("tp")
    fs = lax.axis_index("fs")
    vfac = lax.dynamic_slice_in_dim(value_factor, tp * cols, cols, 0)
    ofac = lax.dynamic_slice_in_dim(output_factor, tp * cols, cols, 0)
    scale = 1.0 / math.sqrt(tokens * nfs)
    flat = width % 128 == 0
    go_shape = (cols, nfs * width) if flat else (nfs, cols, width)
    vmem = pl.BlockSpec(memory_space=pltpu.VMEM)
    hbm = pl.BlockSpec(memory_space=pl.ANY)
    dma = pltpu.SemaphoreType.DMA
    moment = jax.ShapeDtypeStruct((rows, cols), F32)
    gv, go, dfull, own = pl.pallas_call(
        functools.partial(exchange, nfs, ntp, scale),
        out_shape=(
            jax.ShapeDtypeStruct((nfs, width, cols), BF16),
            jax.ShapeDtypeStruct(go_shape, BF16),
            jax.ShapeDtypeStruct((nfs, rows, 2 * cols), BF16),
            jax.ShapeDtypeStruct((rows, 2 * cols), F32),
        ),
        in_specs=[vmem] * 7 + [pl.BlockSpec(memory_space=pltpu.SMEM)] + [vmem] * 7,
        out_specs=(hbm, hbm, hbm, vmem),
        scratch_shapes=[
            pltpu.VMEM((tokens, cols), BF16),
            pltpu.VMEM((ntp, tokens, 2 * rank), F32),
            pltpu.VMEM((nfs, rows, 2 * cols), BF16),
            pltpu.VMEM((nfs, rows, 2 * cols), BF16),
            pltpu.VMEM((rows, 2 * cols), BF16),
            dma((2 * nfs + 1,)), dma((nfs,)), dma((2 * nfs + 1,)), dma((nfs,)),
            dma((ntp,)), dma((ntp,)),
            dma((nfs,)), dma((nfs,)),
            dma((nfs,)), dma((nfs,)), dma((nfs,)), dma((nfs,)), dma((3,)),
        ],
        compiler_params=pltpu.CompilerParams(collective_id=0, has_side_effects=True),
    )(
        encode(value_weight), encode(output_weight),
        inputs, value_cotangent, first_map, second_map, output_cotangent,
        lambdas, head_gain.reshape(1, -1), vfac, ofac,
        value_moment, value_second, output_moment, output_second,
    )
    dirs = dfull.reshape(nfs * rows, 2 * cols)
    same = lambda i: (0, 0)
    if flat:
        o_spec, oc_shape = pl.BlockSpec((cols, width), lambda i: (0, i)), (cols, nfs * width)
    else:
        o_spec, oc_shape = pl.BlockSpec((1, cols, width), lambda i: (i, 0, 0)), go_shape
    small = pl.BlockSpec((rows, cols), same)
    outs = pl.pallas_call(
        functools.partial(update, width),
        grid=(nfs,),
        out_shape=(
            jax.ShapeDtypeStruct((nfs * width, cols), BF16),
            jax.ShapeDtypeStruct(oc_shape, BF16),
            jax.ShapeDtypeStruct((width, cols), F32),
            jax.ShapeDtypeStruct((cols, width), F32),
            moment, moment, moment, moment,
        ),
        in_specs=[
            pl.BlockSpec(memory_space=pltpu.SMEM),
            pl.BlockSpec((1, width, cols), lambda i: (i, 0, 0)),
            o_spec,
            pl.BlockSpec((width, rank), lambda i: (i, 0)),
            pl.BlockSpec((width, rank), lambda i: (i, 0)),
            pl.BlockSpec((rank, cols), lambda i: (0, 0)),
            pl.BlockSpec((rank, cols), lambda i: (0, 1)),
            pl.BlockSpec((width, cols), same),
            pl.BlockSpec((cols, width), same),
            pl.BlockSpec((rows, 2 * cols), same),
            small, small, small, small,
        ],
        out_specs=(
            pl.BlockSpec((width, cols), lambda i: (i, 0)),
            o_spec,
            pl.BlockSpec((width, cols), same),
            pl.BlockSpec((cols, width), same),
            small, small, small, small,
        ),
        scratch_shapes=[pltpu.VMEM((cols, rank), BF16)],
        compiler_params=pltpu.CompilerParams(dimension_semantics=("arbitrary",)),
    )(
        fs.reshape(1), gv, go, value_factor, output_factor, dirs, dirs,
        value_weight, output_weight, own,
        value_moment, value_second, output_moment, output_second,
    )
    value_copy, output_copy, value_master, output_master, *moments = outs
    if not flat:
        output_copy = output_copy.transpose(1, 0, 2).reshape(cols, nfs * width)
    return (value_master, output_master, *moments, value_copy, output_copy)


def solution(mesh):
    both = P("fs", "tp")
    in_specs = (
        both, both, both, both, P("tp"), P(), both, P(), P(), both, P("tp", "fs"),
        both, both, both, both,
    )
    out_specs = (
        both, P("tp", "fs"), both, both, both, both, P(None, "tp"), P("tp", None),
    )
    body = functools.partial(local, mesh.shape["fs"], mesh.shape["tp"])
    return jax.shard_map(
        body, mesh=mesh, in_specs=in_specs, out_specs=out_specs, check_vma=False
    )
```

```python
import functools
import math

import jax
import jax.numpy as jnp
from jax import lax
from jax.experimental import pallas as pl
from jax.experimental.pallas import tpu as pltpu
from jax.sharding import PartitionSpec as P

F32 = jnp.float32
BF16 = jnp.bfloat16


CODE = 2.0**30


def encode(w):
    square = (w * CODE) * (w * CODE)
    fourth = square * square
    return jnp.where(w < 0, -fourth, fourth).astype(BF16)


def decode(v):
    v = v.astype(F32)
    size = lax.rsqrt(lax.rsqrt(jnp.maximum(jnp.abs(v), 1e-36))) * (1.0 / CODE)
    return jnp.where(v < 0, -size, size)


def exchange(
    nfs, ntp, scale,
    vw_in, ow_in, inp_in, ocot_in, first_in, second_in, vcot_in, lam, gain, vfac, ofac,
    vm, vs, om, os_,
    gv, go, dfull, own_out,
    vw, ow, inp, ocot, first, second, vcot, heads, proj, part, got, direction,
    vsend, vrecv, osend, orecv, psend, precv, rsend, rrecv,
    dvsend, dvrecv, dosend, dorecv, lsem, insem,
):
    me = lax.axis_index("fs")
    tp = lax.axis_index("tp")
    cols = inp.shape[1]
    rank = vfac.shape[1]
    nx = 2 if nfs % 2 == 0 else 1
    ny = 2 if nfs % 4 == 0 else 1
    nz = nfs // (nx * ny)
    x = lax.rem(me, nx)
    y = lax.rem(lax.div(me, nx), ny)
    z = lax.div(me, nx * ny)

    def at(dz, dy, dx):
        zz = lax.rem(z + dz, nz)
        yy = lax.rem(y + dy, ny)
        xx = lax.rem(x + dx, nx)
        return (zz * ny + yy) * nx + xx

    barrier = pltpu.get_barrier_semaphore()
    for k in range(1, nfs):
        pl.semaphore_signal(barrier, inc=1, device_id={"fs": lax.rem(me + k, nfs)})
    for k in range(1, ntp):
        pl.semaphore_signal(barrier, inc=1, device_id={"tp": lax.rem(tp + k, ntp)})
    loads = []
    pairs = ((inp_in, inp), (ocot_in, ocot), (first_in, first), (second_in, second), (vcot_in, vcot))
    for k, (src, dst) in enumerate(pairs):
        load = pltpu.make_async_copy(src, dst, insem.at[k])
        load.start()
        loads.append(load)
    vw[...] = encode(vw_in[...])
    ow[...] = encode(ow_in[...])
    pl.semaphore_wait(barrier, nfs + ntp - 2)

    width = vw.shape[0]

    def vslot(b):
        return gv.at[b]

    def oslot(b):
        if len(go.shape) == 2:
            return go.at[:, pl.ds(pl.multiple_of(b * width, width), width)]
        return go.at[b]

    def dvslot(b):
        return dfull.at[b, :, pl.ds(0, cols)]

    def doslot(b):
        return dfull.at[b, :, pl.ds(cols, cols)]

    kinds = {
        "v": (vslot, vsend, vrecv),
        "o": (oslot, osend, orecv),
        "dv": (dvslot, dvsend, dvrecv),
        "do": (doslot, dosend, dorecv),
    }
    pending = []
    counts = {kind: 0 for kind in kinds}

    def when(cond, run):
        if cond is None:
            run()
        else:
            pl.when(cond)(run)

    def send(kind, src, b, target, cond=None):
        k = counts[kind]
        counts[kind] = k + 1
        slot, ss, rs = kinds[kind]

        def make():
            return pltpu.make_async_remote_copy(
                src_ref=slot(b) if src is None else src,
                dst_ref=slot(b),
                send_sem=ss.at[k],
                recv_sem=rs.at[b],
                device_id={"fs": target},
            )

        when(cond, lambda: make().start())
        pending.append((cond, make))

    def arrived(kind, b, cond=None):
        slot, ss, rs = kinds[kind]
        when(cond, lambda: pltpu.make_async_remote_copy(
            src_ref=slot(b), dst_ref=slot(b), send_sem=ss.at[0], recv_sem=rs.at[b],
            device_id={"fs": me},
        ).wait_recv())

    def spread(kind, src, b, cond=None):
        turns = ((ny, (0, 1, 0)), (nx, (0, 0, 1)))
        for extent, turn in turns if kind in ("v", "dv") else turns[::-1]:
            if extent > 1:
                send(kind, src, b, at(*turn), cond)

    def across(kind, bz, cond=None):
        first_turn, second_turn = (ny, nx) if kind in ("v", "dv") else (nx, ny)
        if first_turn == 1:
            return
        if kind in ("v", "dv"):
            b, target = (bz * ny + lax.rem(y + 1, ny)) * nx + x, at(0, 0, 1)
        else:
            b, target = (bz * ny + y) * nx + lax.rem(x + 1, nx), at(0, 1, 0)
        arrived(kind, b, cond)
        if second_turn > 1:
            send(kind, None, b, target, cond)

    def plane(bz):
        return (bz * ny + y) * nx + x

    up, down = lax.rem(z + 1, nz), lax.rem(z + nz - 1, nz)

    def along(kind, s):
        for sign in (1, -1):
            source = z - sign * s
            cond = source >= 0 if sign == 1 else source < nz
            b = plane(lax.rem(source + nz, nz))
            arrived(kind, b, cond)
            if sign == 1:
                send(kind, None, b, plane(up), (source >= 0) & (z + 1 < nz))
            else:
                send(kind, None, b, plane(down), (source < nz) & (z > 0))
            spread(kind, None, b, cond)

    def behind(kind, s):
        for sign in (1, -1):
            source = z - sign * s
            cond = source >= 0 if sign == 1 else source < nz
            across(kind, lax.rem(source + nz, nz), cond)

    own_v = pltpu.make_async_copy(vw, vslot(me), lsem.at[0])
    own_o = pltpu.make_async_copy(ow, oslot(me), lsem.at[1])
    own_v.start()
    own_o.start()
    for kind, src in (("v", vw), ("o", ow)):
        send(kind, src, me, plane(up), z + 1 < nz)
        send(kind, src, me, plane(down), z > 0)
        spread(kind, src, me)

    mine = pl.ds(pl.multiple_of(tp * cols, cols), cols)
    loads[0].wait()
    proj[0, :, :rank] = jnp.dot(inp[...], vfac[mine, :], preferred_element_type=F32)
    loads[1].wait()
    proj[0, :, rank:] = jnp.dot(ocot[...], ofac[mine, :], preferred_element_type=F32)
    pcopies = []
    for k in range(1, ntp):
        copy = pltpu.make_async_remote_copy(
            src_ref=proj.at[0], dst_ref=proj.at[k],
            send_sem=psend.at[k], recv_sem=precv.at[k],
            device_id={"tp": lax.rem(tp + k, ntp)},
        )
        copy.start()
        pcopies.append(copy)

    loads[2].wait()
    loads[3].wait()
    head_width = gain.shape[1]
    for h in range(cols // head_width):
        span = pl.ds(h * head_width, head_width)
        diff = first[:, span].astype(F32) - lam[h] * second[:, span].astype(F32)
        mean = jnp.mean(diff * diff, axis=-1, keepdims=True)
        heads[:, span] = (diff * lax.rsqrt(mean + 1e-06) * gain[...]).astype(BF16)

    for copy in pcopies:
        copy.wait()
    total = proj[0]
    for k in range(1, ntp):
        total = total + proj[k]
    high = total.astype(BF16)
    low = (total - high.astype(F32)).astype(BF16)

    def contract(a, b):
        return lax.dot_general(a, b, (((0,), (0,)), ((), ())), preferred_element_type=F32)

    loads[4].wait()
    rows = vm.shape[0]
    low_v = (contract(high[:, :rank], vcot[...]) + contract(low[:, :rank], vcot[...])) * scale
    part[:, :, :cols] = low_v.astype(BF16).reshape(nfs, rows, cols)
    low_o = (contract(high[:, rank:], heads[...]) + contract(low[:, rank:], heads[...])) * scale
    part[:, :, cols:] = low_o.astype(BF16).reshape(nfs, rows, cols)

    rcopies = []
    for k in range(1, nfs):
        peer = lax.rem(me + k, nfs)
        copy = pltpu.make_async_remote_copy(
            src_ref=part.at[peer], dst_ref=got.at[k],
            send_sem=rsend.at[k], recv_sem=rrecv.at[k],
            device_id={"fs": peer},
        )
        copy.start()
        rcopies.append(copy)

    for s in range(1, nz):
        for kind in ("v", "o"):
            along(kind, s)
        for kind in ("v", "o"):
            if s == 1:
                across(kind, z)
            else:
                behind(kind, s - 1)

    for copy in rcopies:
        copy.wait_recv()
    own = part[me].astype(F32)
    for k in range(1, nfs):
        own = own + got[k].astype(F32)
    own_out[...] = own
    for off, m_ref, s_ref in ((0, vm, vs), (cols, om, os_)):
        g = own[:, off:off + cols]
        m = 0.8 * m_ref[...] + 0.2 * g
        s = 0.95 * s_ref[...] + 0.05 * g * g
        direction[:, off:off + cols] = (m / (jnp.sqrt(s) + 1e-08)).astype(BF16)
    own_d = pltpu.make_async_copy(direction, dfull.at[me], lsem.at[2])
    own_d.start()
    halves = {"dv": direction.at[:, pl.ds(0, cols)], "do": direction.at[:, pl.ds(cols, cols)]}
    for kind, src in halves.items():
        for dz in range(1, nz):
            send(kind, src, me, at(dz, 0, 0))
        spread(kind, src, me)
    for dz in range(1, nz):
        for kind in halves:
            arrived(kind, at(dz, 0, 0))
            spread(kind, None, at(dz, 0, 0))
    for dz in range(nz):
        for kind in halves:
            across(kind, lax.rem(z + dz, nz))
    for kind in ("v", "o"):
        if nz > 1:
            behind(kind, nz - 1)
        else:
            across(kind, z)

    for dz in range(nz):
        for dy in range(ny):
            if nx > 1:
                arrived("v", at(dz, dy, 1))
                arrived("dv", at(dz, dy, 1))
        for dx in range(nx):
            if ny > 1:
                arrived("o", at(dz, 1, dx))
                arrived("do", at(dz, 1, dx))
    for copy in rcopies:
        copy.wait_send()
    for cond, make in pending:
        when(cond, lambda make=make: make().wait_send())
    own_v.wait()
    own_o.wait()
    own_d.wait()


def update(
    width, fs, gv, go, vfac, ofac, dv, do, vw, ow, own, vm, vs, om, os_,
    v_copy, o_copy, v_master, o_master, vm_new, vs_new, om_new, os_new, turned,
):
    step = pl.program_id(0)
    cols = dv.shape[1]

    @pl.when(step == 0)
    def _():
        turned[...] = do[...].T
        for off, m_ref, s_ref, m_out, s_out in (
            (0, vm, vs, vm_new, vs_new),
            (cols, om, os_, om_new, os_new),
        ):
            g = own[:, off:off + cols]
            m_out[...] = 0.8 * m_ref[...] + 0.2 * g
            s_out[...] = 0.95 * s_ref[...] + 0.05 * g * g

    move_v = 0.05 * jnp.dot(vfac[...], dv[...], preferred_element_type=F32)
    move_o = 0.05 * lax.dot_general(
        turned[...], ofac[...], (((1,), (1,)), ((), ())), preferred_element_type=F32
    )
    v_copy[...] = (decode(gv[0]) - move_v).astype(BF16)
    o_old = decode(go[...] if len(go.shape) == 2 else go[0])
    o_new = (o_old - move_o).astype(BF16)
    if len(go.shape) == 2:
        o_copy[...] = o_new
    else:
        o_copy[0] = o_new

    @pl.when(step == fs[0])
    def _():
        v_master[...] = vw[...] - move_v
        o_master[...] = ow[...] - move_o


def local(
    nfs, ntp,
    inputs, value_cotangent, first_map, second_map, lambdas, head_gain,
    output_cotangent, value_factor, output_factor, value_weight, output_weight,
    value_moment, value_second, output_moment, output_second,
):
    tokens, cols = inputs.shape
    width = value_weight.shape[0]
    rank = value_factor.shape[1]
    rows = value_moment.shape[0]
    fs = lax.axis_index("fs")
    scale = 1.0 / math.sqrt(tokens * nfs)
    flat = width % 128 == 0
    go_shape = (cols, nfs * width) if flat else (nfs, cols, width)
    vmem = pl.BlockSpec(memory_space=pltpu.VMEM)
    hbm = pl.BlockSpec(memory_space=pl.ANY)
    dma = pltpu.SemaphoreType.DMA
    moment = jax.ShapeDtypeStruct((rows, cols), F32)
    gv, go, dfull, own = pl.pallas_call(
        functools.partial(exchange, nfs, ntp, scale),
        out_shape=(
            jax.ShapeDtypeStruct((nfs, width, cols), BF16),
            jax.ShapeDtypeStruct(go_shape, BF16),
            jax.ShapeDtypeStruct((nfs, rows, 2 * cols), BF16),
            jax.ShapeDtypeStruct((rows, 2 * cols), F32),
        ),
        in_specs=[vmem] * 2 + [hbm] * 5 + [pl.BlockSpec(memory_space=pltpu.SMEM)] + [vmem] * 7,
        out_specs=(hbm, hbm, hbm, vmem),
        scratch_shapes=[
            pltpu.VMEM((width, cols), BF16),
            pltpu.VMEM((cols, width), BF16),
            *[pltpu.VMEM((tokens, cols), BF16)] * 6,
            pltpu.VMEM((ntp, tokens, 2 * rank), F32),
            pltpu.VMEM((nfs, rows, 2 * cols), BF16),
            pltpu.VMEM((nfs, rows, 2 * cols), BF16),
            pltpu.VMEM((rows, 2 * cols), BF16),
            dma((2 * nfs + 1,)), dma((nfs,)), dma((2 * nfs + 1,)), dma((nfs,)),
            dma((ntp,)), dma((ntp,)),
            dma((nfs,)), dma((nfs,)),
            dma((nfs,)), dma((nfs,)), dma((nfs,)), dma((nfs,)), dma((3,)), dma((5,)),
        ],
        compiler_params=pltpu.CompilerParams(collective_id=0, has_side_effects=True),
    )(
        value_weight, output_weight,
        inputs, output_cotangent, first_map, second_map, value_cotangent,
        lambdas, head_gain.reshape(1, -1), value_factor, output_factor,
        value_moment, value_second, output_moment, output_second,
    )
    dirs = dfull.reshape(nfs * rows, 2 * cols)
    same = lambda i: (0, 0)
    if flat:
        o_spec, oc_shape = pl.BlockSpec((cols, width), lambda i: (0, i)), (cols, nfs * width)
    else:
        o_spec, oc_shape = pl.BlockSpec((1, cols, width), lambda i: (i, 0, 0)), go_shape
    small = pl.BlockSpec((rows, cols), same)
    outs = pl.pallas_call(
        functools.partial(update, width),
        grid=(nfs,),
        out_shape=(
            jax.ShapeDtypeStruct((nfs * width, cols), BF16),
            jax.ShapeDtypeStruct(oc_shape, BF16),
            jax.ShapeDtypeStruct((width, cols), F32),
            jax.ShapeDtypeStruct((cols, width), F32),
            moment, moment, moment, moment,
        ),
        in_specs=[
            pl.BlockSpec(memory_space=pltpu.SMEM),
            pl.BlockSpec((1, width, cols), lambda i: (i, 0, 0)),
            o_spec,
            pl.BlockSpec((width, rank), lambda i: (i, 0)),
            pl.BlockSpec((width, rank), lambda i: (i, 0)),
            pl.BlockSpec((rank, cols), lambda i: (0, 0)),
            pl.BlockSpec((rank, cols), lambda i: (0, 1)),
            pl.BlockSpec((width, cols), same),
            pl.BlockSpec((cols, width), same),
            pl.BlockSpec((rows, 2 * cols), same),
            small, small, small, small,
        ],
        out_specs=(
            pl.BlockSpec((width, cols), lambda i: (i, 0)),
            o_spec,
            pl.BlockSpec((width, cols), same),
            pl.BlockSpec((cols, width), same),
            small, small, small, small,
        ),
        scratch_shapes=[pltpu.VMEM((cols, rank), BF16)],
        compiler_params=pltpu.CompilerParams(dimension_semantics=("arbitrary",)),
    )(
        fs.reshape(1), gv, go, value_factor, output_factor, dirs, dirs,
        value_weight, output_weight, own,
        value_moment, value_second, output_moment, output_second,
    )
    value_copy, output_copy, value_master, output_master, *moments = outs
    if not flat:
        output_copy = output_copy.transpose(1, 0, 2).reshape(cols, nfs * width)
    return (value_master, output_master, *moments, value_copy, output_copy)


def solution(mesh):
    both = P("fs", "tp")
    in_specs = (
        both, both, both, both, P("tp"), P(), both, P(), P(), both, P("tp", "fs"),
        both, both, both, both,
    )
    out_specs = (
        both, P("tp", "fs"), both, both, both, both, P(None, "tp"), P("tp", None),
    )
    body = functools.partial(local, mesh.shape["fs"], mesh.shape["tp"])
    return jax.shard_map(
        body, mesh=mesh, in_specs=in_specs, out_specs=out_specs, check_vma=False
    )
```
